32 devices in a mesh: fs: 8 (over z, y), tp: 4 (over x, core).
Axes of the slice: x: 2, y: 2, z: 4, core: 2. Of those that a mesh axis runs over, the one named last changes fastest.
Arguments:
- tokens: bfloat16 [16, 384, 2048], P('fs', None, 'tp'), may hold values from -34 to 34
- mix_gain: float32 [2048], replicated, may hold values from 0.1 to 1.9
- w_bgate: float32 [2048, 2048], P('fs', 'tp'), may hold values from -0.125 to 0.125
- w_cgate: float32 [2048, 2048], P('fs', 'tp'), may hold values from -0.125 to 0.125
- w_value: float32 [2048, 2048], P('fs', 'tp'), may hold values from -0.125 to 0.125
- in_scale: float32 [3, 2048], P(None, 'tp'), may hold values from 0.5 to 2
- mix_taps: float32 [3, 2048], P(None, 'tp'), may hold values from -3.5 to 3.5
- w_mixout: float32 [2048, 2048], P('tp', 'fs'), may hold values from -0.125 to 0.125
- mixout_scale: float32 [1, 2048], P(None, 'fs'), may hold values from 0.5 to 2
- ffn_gain: float32 [2048], replicated, may hold values from 0.1 to 1.9
- w_upgate: float32 [2048, 5632], P('fs', 'tp'), may hold values from -0.125 to 0.125
- w_upval: float32 [2048, 5632], P('fs', 'tp'), may hold values from -0.125 to 0.125
- up_scale: float32 [2, 5632], P(None, 'tp'), may hold values from 0.5 to 2
- ffn_taps: float32 [2, 3, 5632], P(None, None, 'tp'), may hold values from -3.5 to 3.5
- w_down: float32 [5632, 2048], P('tp', 'fs'), may hold values from -0.078125 to 0.078125
- down_scale: float32 [1, 2048], P(None, 'fs'), may hold values from 0.5 to 2
Outputs:
- layer_out: bfloat16 [16, 384, 2048], P('fs', None, 'tp')
The draws below stay inside these ranges and needn't reach their ends.
All inputs are finite; a program needn't handle non-finite values.
Results may differ from the reference program's by a relative error of at most 0.015.
Values may be sent and summed in bfloat16 or wider, within the bound.
A program may use at most 64 MiB of HBM per device.

```python
import math
import jax
import jax.numpy as jnp
from jax import lax

D = 2048
FF = 5632
CONV = 3
LEN = 384
SEQS = 16
N_TP = 4


def draw_tokens(key, part):
    key_base, key_rows, key_cols = jax.random.split(key, 3)
    base = jax.random.normal(key_base, (SEQS, LEN, D), jnp.float32)
    base = jnp.clip(base, -4.0, 4.0)
    row_scale = jnp.exp(jax.random.uniform(key_rows, (SEQS, LEN, 1), jnp.float32, math.log(0.3), math.log(3.0)))
    rising = jnp.exp(math.log(4.0) * (jnp.arange(D, dtype=jnp.float32) / D - 0.5))
    col_scale = rising * jax.random.uniform(key_cols, (D,), jnp.float32, 0.7, 1.4)
    return (base * row_scale * col_scale).astype(jnp.bfloat16)


def block_levels(own_key, shape, cuts, smallest, high):
    factor_of, own = 1.0, jax.random.fold_in(own_key, 6)
    for position, shards_of in cuts:
        draws = jnp.exp(jax.random.uniform(jax.random.fold_in(own, position), (shards_of,), jnp.float32, smallest / len(cuts), high / len(cuts)))
        factor_of = factor_of * jnp.repeat(draws, shape[position] // shards_of).reshape([-1 if axis == position else 1 for axis in range(len(shape))])
    return factor_of


def gaussian(rng, shape, spread, most, cuts=(), kind=jnp.bfloat16):
    loudness = block_levels(rng, shape, cuts, -0.22, 0.18) if cuts else 1.0
    drawn = jax.random.normal(rng, shape, jnp.float32) * spread * loudness
    return jnp.minimum(jnp.maximum(drawn, -most), most).astype(kind)


def setup_inputs(seed: int = 0) -> dict:
    streams_of = jax.random.split(jax.random.key(seed), 17)
    return {
        "tokens": draw_tokens(jax.random.fold_in(streams_of[16], 71), 0),
        "mix_gain": jnp.clip(1.0 + 0.18 * jax.random.normal(streams_of[1], (D,), jnp.float32), 0.1, 1.9),
        "w_bgate": gaussian(streams_of[2], (D, D), D ** -0.5, 0.125, ((0, 8), (1, 4)), jnp.float32),
        "w_cgate": gaussian(streams_of[3], (D, D), D ** -0.5, 0.125, ((0, 8), (1, 4)), jnp.float32),
        "w_value": gaussian(streams_of[4], (D, D), D ** -0.5, 0.125, ((0, 8), (1, 4)), jnp.float32),
        "in_scale": jnp.clip(jnp.exp(math.log(2.0) - 1.3862944 * jax.random.uniform(streams_of[5], (3, D), jnp.float32) ** block_levels(streams_of[5], (3, D), ((1, 4),), -0.2, 0.2)), 0.5, 2.0),
        "mix_taps": gaussian(streams_of[6], (CONV, D), CONV ** -0.5, 3.5, ((1, 4),), jnp.float32),
        "w_mixout": gaussian(streams_of[7], (D, D), D ** -0.5, 0.125, ((0, 4), (1, 8)), jnp.float32),
        "mixout_scale": jnp.clip(jnp.exp(math.log(2.0) - 1.3862944 * jax.random.uniform(streams_of[8], (1, D), jnp.float32) ** block_levels(streams_of[8], (1, D), ((1, 8),), -0.2, 0.2)), 0.5, 2.0),
        "ffn_gain": jnp.clip(1.0 + 0.18 * jax.random.normal(streams_of[9], (D,), jnp.float32), 0.1, 1.9),
        "w_upgate": gaussian(streams_of[10], (D, FF), D ** -0.5, 0.125, ((0, 8), (1, 4)), jnp.float32),
        "w_upval": gaussian(streams_of[11], (D, FF), D ** -0.5, 0.125, ((0, 8), (1, 4)), jnp.float32),
        "up_scale": jnp.clip(jnp.exp(math.log(2.0) - 1.3862944 * jax.random.uniform(streams_of[12], (2, FF), jnp.float32) ** block_levels(streams_of[12], (2, FF), ((1, 4),), -0.2, 0.2)), 0.5, 2.0),
        "ffn_taps": gaussian(streams_of[13], (2, CONV, FF), CONV ** -0.5, 3.5, ((2, 4),), jnp.float32),
        "w_down": gaussian(streams_of[14], (FF, D), FF ** -0.5, 0.078125, ((0, 4), (1, 8)), jnp.float32),
        "down_scale": jnp.clip(jnp.exp(math.log(2.0) - 1.3862944 * jax.random.uniform(streams_of[15], (1, D), jnp.float32) ** block_levels(streams_of[15], (1, D), ((1, 8),), -0.2, 0.2)), 0.5, 2.0),
    }


EPS = 1e-06

def normed_rows(values, gain):
    floats = values.astype(jnp.float32)
    factor = lax.rsqrt(lax.optimization_barrier(jnp.mean(floats * floats, axis=-1, keepdims=True)) + EPS)
    return (floats * factor * gain).astype(jnp.bfloat16).reshape(SEQS * LEN, D)

def causal_taps(values, taps):
    padded = jnp.pad(values, ((0, 0), (CONV - 1, 0), (0, 0)))
    result = jnp.zeros(values.shape, jnp.float32)
    for offset in range(CONV):
        result = result + padded[:, offset:offset + LEN] * taps[offset]
    return result

def project(inputs, matrix, scale):
    return jnp.dot(inputs, matrix.astype(jnp.bfloat16), preferred_element_type=jnp.float32) * scale

def blocked_sum(inputs, matrix, scale):
    inner_width = inputs.shape[1] // N_TP
    total = jnp.zeros((inputs.shape[0], matrix.shape[1]), jnp.float32)
    for block in range(N_TP):
        lower = block * inner_width
        part_out = jnp.dot(inputs[:, lower:lower + inner_width], matrix[lower:lower + inner_width].astype(jnp.bfloat16), preferred_element_type=jnp.float32) * scale
        rounded = lax.optimization_barrier(part_out.astype(jnp.bfloat16))
        total = total + rounded.astype(jnp.float32)
    return total

def reference(tokens, mix_gain, w_bgate, w_cgate, w_value, in_scale, mix_taps, w_mixout, mixout_scale, ffn_gain, w_upgate, w_upval, up_scale, ffn_taps, w_down, down_scale):
    row_count = SEQS * LEN
    normed = normed_rows(tokens, mix_gain)
    bgate = project(normed, w_bgate, in_scale[0])
    cgate = project(normed, w_cgate, in_scale[1])
    value = project(normed, w_value, in_scale[2])
    inner = (cgate * value).reshape(SEQS, LEN, D)
    convolved = causal_taps(inner, mix_taps)
    gated = (bgate.reshape(SEQS, LEN, D) * convolved).astype(jnp.bfloat16).reshape(row_count, D)
    mix = blocked_sum(gated, w_mixout, mixout_scale)
    resid = (tokens.reshape(row_count, D).astype(jnp.float32) + mix).astype(jnp.bfloat16)
    normed_ffn = normed_rows(resid.reshape(SEQS, LEN, D), ffn_gain)
    gate_pre = project(normed_ffn, w_upgate, up_scale[0]).reshape(SEQS, LEN, FF)
    val_pre = project(normed_ffn, w_upval, up_scale[1]).reshape(SEQS, LEN, FF)
    gate_conv = causal_taps(gate_pre, ffn_taps[0])
    val_conv = causal_taps(val_pre, ffn_taps[1])
    active = (jax.nn.silu(gate_conv) * val_conv).astype(jnp.bfloat16).reshape(row_count, FF)
    ffn = blocked_sum(active, w_down, down_scale)
    layer_out = (resid.astype(jnp.float32) + ffn).astype(jnp.bfloat16)
    return layer_out.reshape(SEQS, LEN, D)
```

```python
import functools

import jax
import jax.numpy as jnp
from jax import lax
from jax.experimental import pallas as pl
from jax.experimental.pallas import tpu as pltpu
from jax.sharding import PartitionSpec as P

EPS = 1e-06
MESH = pl.DeviceIdType.MESH
F32 = jnp.float32
BF16 = jnp.bfloat16
S, A, B, C, D = range(5)


def shifted(values, by):
    rows = lax.broadcasted_iota(jnp.int32, values.shape, 0)
    return jnp.where(rows >= by, pltpu.roll(values, by, 0), 0.0)


def causal_taps(values, taps):
    return shifted(values, 2) * taps[0:1] + shifted(values, 1) * taps[1:2] + values * taps[2:3]


def layer_kernel(
    n, n_tp, seqs, tok, gain1, gain2, iscale, mtaps, uscale, ftaps, w_s, w_a, w_b, w_c, w_d, out,
    buf_s, buf_a, buf_b, buf_c, buf_d, xg, rg, normed, gated, active,
    parts_m, recv_m, parts_d, recv_d,
    ring_send, ring_recv, tok_send, tok_recv, mix_send, mix_recv, res_send, res_recv,
    down_send, down_recv, local_sem,
):
    fs, me = lax.axis_index("fs"), lax.axis_index("tp")
    rows, own = tok.shape
    length = rows // seqs
    bpo = n // n_tp
    bw = own // bpo
    width = own * n_tp
    weights = (w_s, w_a, w_b, w_c, w_d)
    bufs = (buf_s, buf_a, buf_b, buf_c, buf_d)
    hi, lo = n // 2, n - 1 - n // 2

    odd = fs % 2
    pos = (1 - odd) * (fs // 2) + odd * (n - 1 - fs // 2)

    def member(q):
        q = (q + 2 * n) % n
        back = q // (n // 2)
        return (1 - back) * (2 * q) + back * (2 * (n - 1 - q) + 1)

    def hops(h, d):
        return hi if h == d else lo

    def ring(g, h, d, k):
        sign = 1 - 2 * d
        owner = member(pos - sign * (k - 1))
        half = weights[g].shape[0] // 2
        part = pl.ds(h * half, half)
        dst = bufs[g].at[owner, part]
        return pltpu.make_async_remote_copy(
            src_ref=weights[g].at[part] if k == 1 else dst,
            dst_ref=dst,
            send_sem=ring_send.at[g, h, d, k - 1],
            recv_sem=ring_recv.at[g, h, d, k - 1],
            device_id={"fs": member(pos + sign)},
            device_id_type=MESH,
        )

    def begin(g, halves=(0, 1)):
        for h in halves:
            for d in (0, 1):
                ring(g, h, d, 1).start()

    def arrive(g, k, halves=(0, 1)):
        for h in halves:
            for d in (0, 1):
                if k <= hops(h, d):
                    ring(g, h, d, k).wait_recv()
                    if k < hops(h, d):
                        ring(g, h, d, k + 1).start()

    def to_peer(src, dst, send, recv, r):
        return pltpu.make_async_remote_copy(
            src_ref=src, dst_ref=dst, send_sem=send, recv_sem=recv,
            device_id={"tp": (me + r) % n_tp}, device_id_type=MESH,
        )

    barrier = pltpu.get_barrier_semaphore()
    for sign in (1, -1):
        pl.semaphore_signal(
            barrier, inc=1, device_id={"fs": member(pos + sign)}, device_id_type=MESH
        )
    for r in range(1, n_tp):
        pl.semaphore_signal(
            barrier, inc=1, device_id={"tp": (me + r) % n_tp}, device_id_type=MESH
        )
    pl.semaphore_wait(barrier, 1 + n_tp)

    begin(S)
    begin(A)
    tok_copies = [
        to_peer(tok, xg.at[me], tok_send.at[r - 1], tok_recv.at[r - 1], r) for r in range(1, n_tp)
    ]
    for copy in tok_copies:
        copy.start()
    locals_ = [
        pltpu.make_async_copy(weights[g], bufs[g].at[fs], local_sem.at[g]) for g in range(5)
    ]
    for copy in locals_:
        copy.start()
    xg[me] = tok[...]

    def normalize(source, gain):
        tile = 32

        def step(i, carry):
            at = pl.ds(pl.multiple_of(i * tile, tile), tile)
            squares = jnp.zeros((tile, 1), F32)
            for t in range(n_tp):
                piece = source[t, at, :].astype(F32)
                squares = squares + jnp.sum(piece * piece, axis=-1, keepdims=True)
            factor = lax.rsqrt(squares * (1.0 / width) + EPS)
            for t in range(n_tp):
                cols = slice(t * own, (t + 1) * own)
                piece = source[t, at, :].astype(F32)
                normed[at, cols] = (piece * factor * gain[:, cols]).astype(BF16)
            return carry

        lax.fori_loop(0, rows // tile, step, 0)

    arrive(S, 1)
    arrive(A, 1)
    for k in range(2, hi + 1):
        arrive(S, k)
    for k in range(2, hi):
        arrive(A, k)
    begin(B)
    begin(C, (0,))
    for copy in tok_copies:
        copy.wait_recv()
    normalize(xg, gain1)
    arrive(A, hi)
    for copy in locals_:
        copy.wait()

    mixed = min(256, own)

    def mixer(s):
        lines = slice(s * length, (s + 1) * length)

        def step(j, carry):
            def product(i):
                at = pl.ds(pl.multiple_of(i * own + j * mixed, 128), mixed)
                matrix = buf_a[:, :, at].reshape(width, mixed)
                return jnp.dot(normed[lines, :], matrix, preferred_element_type=F32)

            at = pl.ds(pl.multiple_of(j * mixed, 128), mixed)
            scales = iscale[:, at]
            inner = (product(1) * scales[1:2]) * (product(2) * scales[2:3])
            convolved = causal_taps(inner, mtaps[:, at])
            gated[lines, at] = (product(0) * scales[0:1] * convolved).astype(BF16)
            return carry

        lax.fori_loop(0, own // mixed, step, 0)

    for s in range(seqs):
        mixer(s)
        if s == 0:
            arrive(B, 1)
    begin(C, (1,))
    for k in range(2, hi + 1):
        arrive(B, k)

    mix_copies = []
    for r in list(range(1, n_tp)) + [0]:
        for b in range(bpo):
            owner = (me + r) % n_tp * bpo + b
            for s in range(seqs):
                lines = slice(s * length, (s + 1) * length)
                part = jnp.dot(gated[lines, :], buf_b[owner], preferred_element_type=F32)
                parts_m[r * bpo + b, lines, :] = (part * buf_s[owner, 0:1, :]).astype(BF16)
            if r:
                copy = to_peer(
                    parts_m.at[r * bpo + b], recv_m.at[r - 1, b],
                    mix_send.at[r - 1, b], mix_recv.at[r - 1, b], r,
                )
                copy.start()
                mix_copies.append(copy)
    arrive(C, 1)

    for copy in mix_copies:
        copy.wait_recv()
    tile = 64

    def total_of(base, own_part, received, store):
        def step(i, carry):
            at = pl.ds(pl.multiple_of(i * tile, tile), tile)
            for b in range(bpo):
                cols = slice(b * bw, (b + 1) * bw)
                total = own_part(b, at).astype(F32)
                for r in range(1, n_tp):
                    total = total + received[r - 1, b, at, :].astype(F32)
                store(at, cols, (base(at, cols).astype(F32) + total).astype(BF16))
            return carry

        lax.fori_loop(0, rows // tile, step, 0)

    def store_resid(at, cols, values):
        rg[me, at, cols] = values

    total_of(lambda at, cols: tok[at, cols], lambda b, at: parts_m[b, at, :], recv_m, store_resid)
    res_copies = [
        to_peer(rg.at[me], rg.at[me], res_send.at[r - 1], res_recv.at[r - 1], r)
        for r in range(1, n_tp)
    ]
    for copy in res_copies:
        copy.start()
    arrive(C, 2)
    for k in range(3, hi):
        arrive(C, k)
    for copy in res_copies:
        copy.wait_recv()
    begin(D)
    normalize(rg, gain2)
    arrive(C, hi)

    tiles = buf_c.shape[2] // 256

    def up(s):
        lines = slice(s * length, (s + 1) * length)

        def step(j, carry):
            at = pl.ds(pl.multiple_of(j * 256, 256), 256)
            matrix = buf_c[:, :, at].reshape(width, 256)
            both = jnp.dot(normed[lines, :], matrix, preferred_element_type=F32) * uscale[:, at]
            both = causal_taps(both, ftaps[:, at])
            gate, val = both[:, :128], both[:, 128:]
            half = pl.ds(pl.multiple_of(j * 128, 128), 128)
            active[lines, half] = (gate / (1.0 + jnp.exp(-gate)) * val).astype(BF16)
            return carry

        lax.fori_loop(0, tiles, step, 0)

    for s in range(seqs):
        up(s)
        if s == 0:
            arrive(D, 1)

    def down(owner):
        t = owner // bpo
        r = (t - me + n_tp) % n_tp
        b = owner % bpo
        for s in range(seqs):
            lines = slice(s * length, (s + 1) * length)
            part = jnp.dot(active[lines, :], buf_d[owner], preferred_element_type=F32)
            parts_d[owner, lines, :] = (part * buf_s[owner, 1:2, :]).astype(BF16)

        @pl.when(r != 0)
        def _():
            pltpu.make_async_remote_copy(
                src_ref=parts_d.at[owner], dst_ref=recv_d.at[r - 1, b],
                send_sem=down_send.at[owner], recv_sem=down_recv.at[r - 1, b],
                device_id={"tp": t}, device_id_type=MESH,
            ).start()

    down(fs)
    for k in range(1, hi + 1):
        if k > 1:
            arrive(D, k)
        if k == 1:
            down(member(pos - 1))
            down(member(pos + 1))
        elif k > 1:
            down(member(pos - k))
            if (2 * k) % n:
                down(member(pos + k))

    ends = []
    for r in range(1, n_tp):
        for b in range(bpo):
            owner = (me + r) % n_tp * bpo + b
            ends.append(
                to_peer(
                    parts_d.at[owner], recv_d.at[r - 1, b],
                    down_send.at[owner], down_recv.at[r - 1, b], r,
                )
            )
    for copy in ends:
        copy.wait_recv()

    def store_out(at, cols, values):
        out[at, cols] = values

    total_of(
        lambda at, cols: rg[me, at, cols], lambda b, at: parts_d[me * bpo + b, at, :], recv_d,
        store_out,
    )

    for copy in tok_copies + mix_copies + res_copies + ends:
        copy.wait_send()
    for g in range(5):
        for h in (0, 1):
            for d in (0, 1):
                for k in range(1, hops(h, d) + 1):
                    ring(g, h, d, k).wait_send()


def on_device(
    n,
    n_tp,
    tokens,
    mix_gain,
    w_bgate,
    w_cgate,
    w_value,
    in_scale,
    mix_taps,
    w_mixout,
    mixout_scale,
    ffn_gain,
    w_upgate,
    w_upval,
    up_scale,
    ffn_taps,
    w_down,
    down_scale,
):
    seqs, length, own = tokens.shape
    rows = seqs * length
    width = own * n_tp
    part = w_bgate.shape[0]
    ff = w_upgate.shape[1]
    pad = -ff % 128
    ffp = ff + pad
    tiles = ffp // 128
    bw = w_mixout.shape[1]

    def interleaved(gate, val):
        pair = [jnp.pad(x, ((0, 0), (0, pad))).reshape(x.shape[0], tiles, 128) for x in (gate, val)]
        return jnp.stack(pair, axis=2).reshape(gate.shape[0], tiles * 256)

    w_s = jnp.concatenate([mixout_scale, down_scale, jnp.zeros((14, bw), F32)], axis=0)
    w_a = jnp.concatenate([w.astype(BF16) for w in (w_bgate, w_cgate, w_value)], axis=1)
    w_b = w_mixout.astype(BF16)
    w_c = interleaved(w_upgate.astype(BF16), w_upval.astype(BF16))
    w_d = jnp.pad(w_down.astype(BF16), ((0, pad), (0, 0)))
    uscale = interleaved(up_scale[0:1], up_scale[1:2])
    ftaps = interleaved(ffn_taps[0], ffn_taps[1])
    weights = (w_s, w_a, w_b, w_c, w_d)
    bpo = n // n_tp
    hi = n // 2
    vmem, dma = pltpu.VMEM, pltpu.SemaphoreType.DMA
    result = pl.pallas_call(
        functools.partial(layer_kernel, n, n_tp, seqs),
        out_shape=jax.ShapeDtypeStruct((rows, own), BF16),
        in_specs=[pl.BlockSpec(memory_space=pltpu.VMEM)] * 7
        + [pl.BlockSpec(memory_space=pl.ANY)] * 5,
        out_specs=pl.BlockSpec(memory_space=pltpu.VMEM),
        scratch_shapes=[vmem((n, *w.shape), w.dtype) for w in weights]
        + [
            vmem((n_tp, rows, own), BF16),
            vmem((n_tp, rows, own), BF16),
            vmem((rows, width), BF16),
            vmem((rows, own), BF16),
            vmem((rows, ffp), BF16),
            vmem((n, rows, bw), BF16),
            vmem((n_tp - 1, bpo, rows, bw), BF16),
            vmem((n, rows, bw), BF16),
            vmem((n_tp - 1, bpo, rows, bw), BF16),
            dma((5, 2, 2, hi)),
            dma((5, 2, 2, hi)),
            dma((n_tp - 1,)),
            dma((n_tp - 1,)),
            dma((n_tp - 1, bpo)),
            dma((n_tp - 1, bpo)),
            dma((n_tp - 1,)),
            dma((n_tp - 1,)),
            dma((n,)),
            dma((n_tp - 1, bpo)),
            dma((5,)),
        ],
        compiler_params=pltpu.CompilerParams(
            collective_id=0, has_side_effects=True, vmem_limit_bytes=67043328
        ),
        name="layer",
    )(
        tokens.reshape(rows, own), mix_gain.reshape(1, width), ffn_gain.reshape(1, width),
        in_scale, mix_taps, uscale, ftaps, *weights,
    )
    return result.reshape(seqs, length, own)


def solution(mesh):
    in_specs = (
        P("fs", None, "tp"),
        P(),
        P("fs", "tp"),
        P("fs", "tp"),
        P("fs", "tp"),
        P(None, "tp"),
        P(None, "tp"),
        P("tp", "fs"),
        P(None, "fs"),
        P(),
        P("fs", "tp"),
        P("fs", "tp"),
        P(None, "tp"),
        P(None, None, "tp"),
        P("tp", "fs"),
        P(None, "fs"),
    )
    out_specs = P("fs", None, "tp")
    body = functools.partial(on_device, mesh.shape["fs"], mesh.shape["tp"])
    return jax.shard_map(body, mesh=mesh, in_specs=in_specs, out_specs=out_specs, check_vma=False)
```

```python
import functools

import jax
import jax.numpy as jnp
from jax import lax
from jax.experimental import pallas as pl
from jax.experimental.pallas import tpu as pltpu
from jax.sharding import PartitionSpec as P

EPS = 1e-06
MESH = pl.DeviceIdType.MESH
F32 = jnp.float32
BF16 = jnp.bfloat16
S, A, B, C, D = range(5)


def shifted(values, by):
    rows = lax.broadcasted_iota(jnp.int32, values.shape, 0)
    return jnp.where(rows >= by, pltpu.roll(values, by, 0), 0.0)


def causal_taps(values, taps):
    return shifted(values, 2) * taps[0:1] + shifted(values, 1) * taps[1:2] + values * taps[2:3]


def layer_kernel(
    n, n_tp, seqs, tok, gain1, gain2, iscale, mtaps, uscale, ftaps, mscale, dscale,
    w_bgate, w_cgate, w_value, w_mixout, w_upgate, w_upval, w_down, out,
    buf_s, buf_a, buf_b, buf_c, buf_d, f_bgate, f_cgate, f_value, f_mixout, f_upgate, f_upval,
    f_down, xg, rg, normed, gated, active,
    parts_m, recv_m, parts_d, recv_d,
    ring_send, ring_recv, tok_send, tok_recv, mix_send, mix_recv, res_send, res_recv,
    down_send, down_recv, local_sem,
):
    fs, me = lax.axis_index("fs"), lax.axis_index("tp")
    rows, own = tok.shape
    length = rows // seqs
    bpo = n // n_tp
    bw = own // bpo
    width = own * n_tp
    bufs = (buf_s, buf_a, buf_b, buf_c, buf_d)
    hi, lo = n // 2, n - 1 - n // 2

    odd = fs % 2
    pos = (1 - odd) * (fs // 2) + odd * (n - 1 - fs // 2)

    def member(q):
        q = (q + 2 * n) % n
        back = q // (n // 2)
        return (1 - back) * (2 * q) + back * (2 * (n - 1 - q) + 1)

    def hops(h, d):
        return hi if h == d else lo

    def ring(g, h, d, k):
        sign = 1 - 2 * d
        owner = member(pos - sign * (k - 1))
        half = bufs[g].shape[1] // 2
        piece = bufs[g].at[owner, pl.ds(h * half, half)]
        return pltpu.make_async_remote_copy(
            src_ref=piece,
            dst_ref=piece,
            send_sem=ring_send.at[g, h, d, k - 1],
            recv_sem=ring_recv.at[g, h, d, k - 1],
            device_id={"fs": member(pos + sign)},
            device_id_type=MESH,
        )

    def begin(g, halves=(0, 1)):
        for h in halves:
            for d in (0, 1):
                ring(g, h, d, 1).start()

    def arrive(g, k, halves=(0, 1)):
        for h in halves:
            for d in (0, 1):
                if k <= hops(h, d):
                    ring(g, h, d, k).wait_recv()
                    if k < hops(h, d):
                        ring(g, h, d, k + 1).start()

    def to_peer(src, dst, send, recv, r):
        return pltpu.make_async_remote_copy(
            src_ref=src, dst_ref=dst, send_sem=send, recv_sem=recv,
            device_id={"tp": (me + r) % n_tp}, device_id_type=MESH,
        )

    sources = (w_bgate, w_cgate, w_value, w_mixout, w_upgate, w_upval, w_down)
    floats = (f_bgate, f_cgate, f_value, f_mixout, f_upgate, f_upval, f_down)
    loads = [
        pltpu.make_async_copy(source, held, local_sem.at[i])
        for i, (source, held) in enumerate(zip(sources, floats))
    ]
    for copy in loads:
        copy.start()

    def cast_rows(held, put):
        tile = 32

        def step(i, carry):
            at = pl.ds(pl.multiple_of(i * tile, tile), tile)
            put(at, held[at, :].astype(BF16))
            return carry

        lax.fori_loop(0, held.shape[0] // tile, step, 0)

    def put_in(i):
        def put(at, values):
            buf_a[fs, at, i * own : (i + 1) * own] = values

        return put

    def put_up(i):
        def put(at, values):
            for j in range(values.shape[1] // 128):
                to = j * 256 + i * 128
                buf_c[fs, at, to : to + 128] = values[:, j * 128 : (j + 1) * 128]

        return put

    def put_mixout(at, values):
        buf_b[fs, at, :] = values

    def put_down(at, values):
        buf_d[fs, at, :] = values

    buf_s[fs] = jnp.zeros(buf_s.shape[1:], F32)
    buf_s[fs, 0:1, :] = mscale[...]
    buf_s[fs, 1:2, :] = dscale[...]
    for i in range(3):
        loads[i].wait()
        cast_rows(floats[i], put_in(i))

    barrier = pltpu.get_barrier_semaphore()
    for sign in (1, -1):
        pl.semaphore_signal(
            barrier, inc=1, device_id={"fs": member(pos + sign)}, device_id_type=MESH
        )
    for r in range(1, n_tp):
        pl.semaphore_signal(
            barrier, inc=1, device_id={"tp": (me + r) % n_tp}, device_id_type=MESH
        )
    pl.semaphore_wait(barrier, 1 + n_tp)

    begin(S)
    begin(A)
    tok_copies = [
        to_peer(tok, xg.at[me], tok_send.at[r - 1], tok_recv.at[r - 1], r) for r in range(1, n_tp)
    ]
    for copy in tok_copies:
        copy.start()
    xg[me] = tok[...]
    for copy in loads[3:]:
        copy.wait()
    cast_rows(f_mixout, put_mixout)
    cast_rows(f_upgate, put_up(0))
    cast_rows(f_upval, put_up(1))

    def normalize(source, gain):
        tile = 32

        def step(i, carry):
            at = pl.ds(pl.multiple_of(i * tile, tile), tile)
            squares = jnp.zeros((tile, 1), F32)
            for t in range(n_tp):
                piece = source[t, at, :].astype(F32)
                squares = squares + jnp.sum(piece * piece, axis=-1, keepdims=True)
            factor = lax.rsqrt(squares * (1.0 / width) + EPS)
            for t in range(n_tp):
                cols = slice(t * own, (t + 1) * own)
                piece = source[t, at, :].astype(F32)
                normed[at, cols] = (piece * factor * gain[:, cols]).astype(BF16)
            return carry

        lax.fori_loop(0, rows // tile, step, 0)

    arrive(S, 1)
    arrive(A, 1)
    cast_rows(f_down, put_down)
    for k in range(2, hi + 1):
        arrive(S, k)
    for k in range(2, hi):
        arrive(A, k)
    begin(B)
    begin(C, (0,))
    for copy in tok_copies:
        copy.wait_recv()
    normalize(xg, gain1)
    arrive(A, hi)

    mixed = min(256, own)

    def mixer(s):
        lines = slice(s * length, (s + 1) * length)

        def step(j, carry):
            def product(i):
                at = pl.ds(pl.multiple_of(i * own + j * mixed, 128), mixed)
                matrix = buf_a[:, :, at].reshape(width, mixed)
                return jnp.dot(normed[lines, :], matrix, preferred_element_type=F32)

            at = pl.ds(pl.multiple_of(j * mixed, 128), mixed)
            scales = iscale[:, at]
            inner = (product(1) * scales[1:2]) * (product(2) * scales[2:3])
            convolved = causal_taps(inner, mtaps[:, at])
            gated[lines, at] = (product(0) * scales[0:1] * convolved).astype(BF16)
            return carry

        lax.fori_loop(0, own // mixed, step, 0)

    for s in range(seqs):
        mixer(s)
        if s == 0:
            arrive(B, 1)
    begin(C, (1,))
    for k in range(2, hi + 1):
        arrive(B, k)

    mix_copies = []
    for r in list(range(1, n_tp)) + [0]:
        for b in range(bpo):
            owner = (me + r) % n_tp * bpo + b
            for s in range(seqs):
                lines = slice(s * length, (s + 1) * length)
                part = jnp.dot(gated[lines, :], buf_b[owner], preferred_element_type=F32)
                parts_m[r * bpo + b, lines, :] = (part * buf_s[owner, 0:1, :]).astype(BF16)
            if r:
                copy = to_peer(
                    parts_m.at[r * bpo + b], recv_m.at[r - 1, b],
                    mix_send.at[r - 1, b], mix_recv.at[r - 1, b], r,
                )
                copy.start()
                mix_copies.append(copy)
    arrive(C, 1)

    for copy in mix_copies:
        copy.wait_recv()
    tile = 64

    def total_of(base, own_part, received, store):
        def step(i, carry):
            at = pl.ds(pl.multiple_of(i * tile, tile), tile)
            for b in range(bpo):
                cols = slice(b * bw, (b + 1) * bw)
                total = own_part(b, at).astype(F32)
                for r in range(1, n_tp):
                    total = total + received[r - 1, b, at, :].astype(F32)
                store(at, cols, (base(at, cols).astype(F32) + total).astype(BF16))
            return carry

        lax.fori_loop(0, rows // tile, step, 0)

    def store_resid(at, cols, values):
        rg[me, at, cols] = values

    total_of(lambda at, cols: tok[at, cols], lambda b, at: parts_m[b, at, :], recv_m, store_resid)
    res_copies = [
        to_peer(rg.at[me], rg.at[me], res_send.at[r - 1], res_recv.at[r - 1], r)
        for r in range(1, n_tp)
    ]
    for copy in res_copies:
        copy.start()
    arrive(C, 2)
    for k in range(3, hi):
        arrive(C, k)
    for copy in res_copies:
        copy.wait_recv()
    begin(D)
    normalize(rg, gain2)
    arrive(C, hi)

    tiles = buf_c.shape[2] // 256

    def up(s):
        lines = slice(s * length, (s + 1) * length)

        def step(j, carry):
            at = pl.ds(pl.multiple_of(j * 256, 256), 256)
            matrix = buf_c[:, :, at].reshape(width, 256)
            both = jnp.dot(normed[lines, :], matrix, preferred_element_type=F32)
            half = pl.ds(pl.multiple_of(j * 128, 128), 128)
            gate = causal_taps(both[:, :128] * uscale[0:1, half], ftaps[0, :, half])
            val = causal_taps(both[:, 128:] * uscale[1:2, half], ftaps[1, :, half])
            active[lines, half] = (gate / (1.0 + jnp.exp(-gate)) * val).astype(BF16)
            return carry

        lax.fori_loop(0, tiles, step, 0)

    for s in range(seqs):
        up(s)
        if s == 0:
            arrive(D, 1)

    def down(owner):
        t = owner // bpo
        r = (t - me + n_tp) % n_tp
        b = owner % bpo
        for s in range(seqs):
            lines = slice(s * length, (s + 1) * length)
            part = jnp.dot(active[lines, :], buf_d[owner], preferred_element_type=F32)
            parts_d[owner, lines, :] = (part * buf_s[owner, 1:2, :]).astype(BF16)

            @pl.when(r != 0)
            def _():
                pltpu.make_async_remote_copy(
                    src_ref=parts_d.at[owner, lines], dst_ref=recv_d.at[r - 1, b, lines],
                    send_sem=down_send.at[owner, s], recv_sem=down_recv.at[r - 1, b, s],
                    device_id={"tp": t}, device_id_type=MESH,
                ).start()

    arrive(D, 2)
    down(fs)
    for k in range(1, hi + 1):
        if k > 2:
            arrive(D, k)
        down(member(pos - k))
        if (2 * k) % n:
            down(member(pos + k))

    ends = []
    for r in range(1, n_tp):
        for b in range(bpo):
            owner = (me + r) % n_tp * bpo + b
            for s in range(seqs):
                lines = slice(s * length, (s + 1) * length)
                ends.append(
                    to_peer(
                        parts_d.at[owner, lines], recv_d.at[r - 1, b, lines],
                        down_send.at[owner, s], down_recv.at[r - 1, b, s], r,
                    )
                )
    for copy in ends:
        copy.wait_recv()

    def store_out(at, cols, values):
        out[at, cols] = values

    total_of(
        lambda at, cols: rg[me, at, cols], lambda b, at: parts_d[me * bpo + b, at, :], recv_d,
        store_out,
    )

    for copy in tok_copies + mix_copies + res_copies + ends:
        copy.wait_send()
    for g in range(5):
        for h in (0, 1):
            for d in (0, 1):
                for k in range(1, hops(h, d) + 1):
                    ring(g, h, d, k).wait_send()


def on_device(
    n,
    n_tp,
    tokens,
    mix_gain,
    w_bgate,
    w_cgate,
    w_value,
    in_scale,
    mix_taps,
    w_mixout,
    mixout_scale,
    ffn_gain,
    w_upgate,
    w_upval,
    up_scale,
    ffn_taps,
    w_down,
    down_scale,
):
    seqs, length, own = tokens.shape
    rows = seqs * length
    width = own * n_tp
    part = w_bgate.shape[0]
    ff = w_upgate.shape[1]
    pad = -ff % 128
    ffp = ff + pad
    bw = w_mixout.shape[1]

    if pad:
        w_upgate, w_upval, up_scale, ffn_taps = (
            jnp.pad(x, [(0, 0)] * (x.ndim - 1) + [(0, pad)])
            for x in (w_upgate, w_upval, up_scale, ffn_taps)
        )
        w_down = jnp.pad(w_down, ((0, pad), (0, 0)))
    weights = (w_bgate, w_cgate, w_value, w_mixout, w_upgate, w_upval, w_down)
    held = [(16, bw), (part, 3 * own), w_mixout.shape, (part, 2 * ffp), w_down.shape]
    bpo = n // n_tp
    hi = n // 2
    vmem, dma = pltpu.VMEM, pltpu.SemaphoreType.DMA
    result = pl.pallas_call(
        functools.partial(layer_kernel, n, n_tp, seqs),
        out_shape=jax.ShapeDtypeStruct((rows, own), BF16),
        in_specs=[pl.BlockSpec(memory_space=pltpu.VMEM)] * 9
        + [pl.BlockSpec(memory_space=pl.ANY)] * 7,
        out_specs=pl.BlockSpec(memory_space=pltpu.VMEM),
        scratch_shapes=[vmem((n, *shape), BF16 if i else F32) for i, shape in enumerate(held)]
        + [vmem(w.shape, F32) for w in weights]
        + [
            vmem((n_tp, rows, own), BF16),
            vmem((n_tp, rows, own), BF16),
            vmem((rows, width), BF16),
            vmem((rows, own), BF16),
            vmem((rows, ffp), BF16),
            vmem((n, rows, bw), BF16),
            vmem((n_tp - 1, bpo, rows, bw), BF16),
            vmem((n, rows, bw), BF16),
            vmem((n_tp - 1, bpo, rows, bw), BF16),
            dma((5, 2, 2, hi)),
            dma((5, 2, 2, hi)),
            dma((n_tp - 1,)),
            dma((n_tp - 1,)),
            dma((n_tp - 1, bpo)),
            dma((n_tp - 1, bpo)),
            dma((n_tp - 1,)),
            dma((n_tp - 1,)),
            dma((n, seqs)),
            dma((n_tp - 1, bpo, seqs)),
            dma((7,)),
        ],
        compiler_params=pltpu.CompilerParams(
            collective_id=0, has_side_effects=True, vmem_limit_bytes=67043328
        ),
        name="layer",
    )(
        tokens.reshape(rows, own), mix_gain.reshape(1, width), ffn_gain.reshape(1, width),
        in_scale, mix_taps, up_scale, ffn_taps, mixout_scale, down_scale, *weights,
    )
    return result.reshape(seqs, length, own)


def solution(mesh):
    in_specs = (
        P("fs", None, "tp"),
        P(),
        P("fs", "tp"),
        P("fs", "tp"),
        P("fs", "tp"),
        P(None, "tp"),
        P(None, "tp"),
        P("tp", "fs"),
        P(None, "fs"),
        P(),
        P("fs", "tp"),
        P("fs", "tp"),
        P(None, "tp"),
        P(None, None, "tp"),
        P("tp", "fs"),
        P(None, "fs"),
    )
    out_specs = P("fs", None, "tp")
    body = functools.partial(on_device, mesh.shape["fs"], mesh.shape["tp"])
    return jax.shard_map(body, mesh=mesh, in_specs=in_specs, out_specs=out_specs, check_vma=False)
```

```python
import functools

import jax
import jax.numpy as jnp
from jax import lax
from jax.experimental import pallas as pl
from jax.experimental.pallas import tpu as pltpu
from jax.sharding import PartitionSpec as P

EPS = 1e-06
MESH = pl.DeviceIdType.MESH
F32 = jnp.float32
BF16 = jnp.bfloat16
S, A, B, C, D = range(5)


def shifted(values, by):
    rows = lax.broadcasted_iota(jnp.int32, values.shape, 0)
    return jnp.where(rows >= by, pltpu.roll(values, by, 0), 0.0)


def causal_taps(values, taps):
    return shifted(values, 2) * taps[0:1] + shifted(values, 1) * taps[1:2] + values * taps[2:3]


def layer_kernel(
    n, n_tp, seqs, tok, gain1, gain2, iscale, mtaps, uscale, ftaps, mscale, dscale,
    w_bgate, w_cgate, w_value, w_mixout, w_upgate, w_upval, w_down, out,
    buf_s, buf_a, buf_b, buf_c, buf_d, f_bgate, f_cgate, f_value, f_mixout, f_upgate, f_upval,
    f_down, xg, rg, normed, gated, active,
    parts_m, recv_m, parts_d, recv_d,
    ring_send, ring_recv, tok_send, tok_recv, mix_send, mix_recv, res_send, res_recv,
    down_send, down_recv, local_sem,
):
    fs, me = lax.axis_index("fs"), lax.axis_index("tp")
    rows, own = tok.shape
    length = rows // seqs
    bpo = n // n_tp
    bw = own // bpo
    width = own * n_tp
    bufs = (buf_s, buf_a, buf_b, buf_c, buf_d)
    hi, lo = n // 2, n - 1 - n // 2

    odd = fs % 2
    pos = (1 - odd) * (fs // 2) + odd * (n - 1 - fs // 2)

    def member(q):
        q = (q + 2 * n) % n
        back = q // (n // 2)
        return (1 - back) * (2 * q) + back * (2 * (n - 1 - q) + 1)

    def hops(h, d):
        return hi if h == d else lo

    def ring(g, h, d, k):
        sign = 1 - 2 * d
        owner = member(pos - sign * (k - 1))
        half = bufs[g].shape[1] // 2
        piece = bufs[g].at[owner, pl.ds(h * half, half)]
        return pltpu.make_async_remote_copy(
            src_ref=piece,
            dst_ref=piece,
            send_sem=ring_send.at[g, h, d, k - 1],
            recv_sem=ring_recv.at[g, h, d, k - 1],
            device_id={"fs": member(pos + sign)},
            device_id_type=MESH,
        )

    def begin(g, halves=(0, 1)):
        for h in halves:
            for d in (0, 1):
                ring(g, h, d, 1).start()

    def arrive(g, k, halves=(0, 1)):
        for h in halves:
            for d in (0, 1):
                if k <= hops(h, d):
                    ring(g, h, d, k).wait_recv()
                    if k < hops(h, d):
                        ring(g, h, d, k + 1).start()

    def to_peer(src, dst, send, recv, r):
        return pltpu.make_async_remote_copy(
            src_ref=src, dst_ref=dst, send_sem=send, recv_sem=recv,
            device_id={"tp": (me + r) % n_tp}, device_id_type=MESH,
        )

    sources = (w_bgate, w_cgate, w_value, w_mixout, w_upgate, w_upval, w_down)
    floats = (f_bgate, f_cgate, f_value, f_mixout, f_upgate, f_upval, f_down)
    loads = [
        pltpu.make_async_copy(source, held, local_sem.at[i])
        for i, (source, held) in enumerate(zip(sources, floats))
    ]
    for copy in loads:
        copy.start()

    def cast_rows(held, put):
        tile = 32

        def step(i, carry):
            at = pl.ds(pl.multiple_of(i * tile, tile), tile)
            put(at, held[at, :].astype(BF16))
            return carry

        lax.fori_loop(0, held.shape[0] // tile, step, 0)

    def put_in(i):
        def put(at, values):
            buf_a[fs, at, i * own : (i + 1) * own] = values

        return put

    def put_up(i):
        def put(at, values):
            for j in range(values.shape[1] // 128):
                to = j * 256 + i * 128
                buf_c[fs, at, to : to + 128] = values[:, j * 128 : (j + 1) * 128]

        return put

    def put_mixout(at, values):
        buf_b[fs, at, :] = values

    def put_down(at, values):
        buf_d[fs, at, :] = values

    buf_s[fs] = jnp.zeros(buf_s.shape[1:], F32)
    buf_s[fs, 0:1, :] = mscale[...]
    buf_s[fs, 1:2, :] = dscale[...]
    for i in range(3):
        loads[i].wait()
        cast_rows(floats[i], put_in(i))

    barrier = pltpu.get_barrier_semaphore()
    for sign in (1, -1):
        pl.semaphore_signal(
            barrier, inc=1, device_id={"fs": member(pos + sign)}, device_id_type=MESH
        )
    for r in range(1, n_tp):
        pl.semaphore_signal(
            barrier, inc=1, device_id={"tp": (me + r) % n_tp}, device_id_type=MESH
        )
    pl.semaphore_wait(barrier, 1 + n_tp)

    begin(S)
    begin(A)
    tok_copies = [
        to_peer(tok, xg.at[me], tok_send.at[r - 1], tok_recv.at[r - 1], r) for r in range(1, n_tp)
    ]
    for copy in tok_copies:
        copy.start()
    xg[me] = tok[...]
    for copy in loads[3:]:
        copy.wait()
    cast_rows(f_mixout, put_mixout)
    cast_rows(f_upgate, put_up(0))
    cast_rows(f_upval, put_up(1))

    def normalize(source, gain):
        tile = 32

        def step(i, carry):
            at = pl.ds(pl.multiple_of(i * tile, tile), tile)
            squares = jnp.zeros((tile, 1), F32)
            for t in range(n_tp):
                piece = source[t, at, :].astype(F32)
                squares = squares + jnp.sum(piece * piece, axis=-1, keepdims=True)
            factor = lax.rsqrt(squares * (1.0 / width) + EPS)
            for t in range(n_tp):
                cols = slice(t * own, (t + 1) * own)
                piece = source[t, at, :].astype(F32)
                normed[at, cols] = (piece * factor * gain[:, cols]).astype(BF16)
            return carry

        lax.fori_loop(0, rows // tile, step, 0)

    arrive(S, 1)
    arrive(A, 1)
    cast_rows(f_down, put_down)
    for k in range(2, hi + 1):
        arrive(S, k)
    for k in range(2, hi):
        arrive(A, k)
    begin(B)
    begin(C, (0,))
    for copy in tok_copies:
        copy.wait_recv()
    normalize(xg, gain1)
    arrive(A, hi)

    mixed = min(256, own)

    def mixer(s):
        lines = slice(s * length, (s + 1) * length)

        def step(j, carry):
            def product(i):
                at = pl.ds(pl.multiple_of(i * own + j * mixed, 128), mixed)
                matrix = buf_a[:, :, at].reshape(width, mixed)
                return jnp.dot(normed[lines, :], matrix, preferred_element_type=F32)

            at = pl.ds(pl.multiple_of(j * mixed, 128), mixed)
            scales = iscale[:, at]
            inner = (product(1) * scales[1:2]) * (product(2) * scales[2:3])
            convolved = causal_taps(inner, mtaps[:, at])
            gated[lines, at] = (product(0) * scales[0:1] * convolved).astype(BF16)
            return carry

        lax.fori_loop(0, own // mixed, step, 0)

    for s in range(seqs):
        mixer(s)
        if s == 0:
            arrive(B, 1)
    begin(C, (1,))
    for k in range(2, hi):
        arrive(B, k)
    arrive(C, 1, (0,))
    arrive(B, hi)
    arrive(C, 1, (1,))

    mix_copies = []
    for r in list(range(1, n_tp)) + [0]:
        for b in range(bpo):
            owner = (me + r) % n_tp * bpo + b
            for s in range(seqs):
                lines = slice(s * length, (s + 1) * length)
                part = jnp.dot(gated[lines, :], buf_b[owner], preferred_element_type=F32)
                parts_m[r * bpo + b, lines, :] = (part * buf_s[owner, 0:1, :]).astype(BF16)
            if r:
                copy = to_peer(
                    parts_m.at[r * bpo + b], recv_m.at[r - 1, b],
                    mix_send.at[r - 1, b], mix_recv.at[r - 1, b], r,
                )
                copy.start()
                mix_copies.append(copy)
    arrive(C, 2, (0,))

    for copy in mix_copies:
        copy.wait_recv()
    tile = 64

    def total_of(base, own_part, received, store):
        def step(i, carry):
            at = pl.ds(pl.multiple_of(i * tile, tile), tile)
            for b in range(bpo):
                cols = slice(b * bw, (b + 1) * bw)
                total = own_part(b, at).astype(F32)
                for r in range(1, n_tp):
                    total = total + received[r - 1, b, at, :].astype(F32)
                store(at, cols, (base(at, cols).astype(F32) + total).astype(BF16))
            return carry

        lax.fori_loop(0, rows // tile, step, 0)

    def store_resid(at, cols, values):
        rg[me, at, cols] = values

    total_of(lambda at, cols: tok[at, cols], lambda b, at: parts_m[b, at, :], recv_m, store_resid)
    res_copies = [
        to_peer(rg.at[me], rg.at[me], res_send.at[r - 1], res_recv.at[r - 1], r)
        for r in range(1, n_tp)
    ]
    for copy in res_copies:
        copy.start()
    arrive(C, 2, (1,))
    for k in range(3, hi):
        arrive(C, k)
    begin(D)
    for copy in res_copies:
        copy.wait_recv()
    normalize(rg, gain2)
    arrive(C, hi)

    tiles = buf_c.shape[2] // 256

    def up(s):
        lines = slice(s * length, (s + 1) * length)

        def step(j, carry):
            at = pl.ds(pl.multiple_of(j * 256, 256), 256)
            matrix = buf_c[:, :, at].reshape(width, 256)
            both = jnp.dot(normed[lines, :], matrix, preferred_element_type=F32)
            half = pl.ds(pl.multiple_of(j * 128, 128), 128)
            gate = causal_taps(both[:, :128] * uscale[0:1, half], ftaps[0, :, half])
            val = causal_taps(both[:, 128:] * uscale[1:2, half], ftaps[1, :, half])
            active[lines, half] = (gate / (1.0 + jnp.exp(-gate)) * val).astype(BF16)
            return carry

        lax.fori_loop(0, tiles, step, 0)

    for s in range(seqs):
        up(s)
        if s == 0:
            arrive(D, 1)

    def down(owner):
        t = owner // bpo
        r = (t - me + n_tp) % n_tp
        b = owner % bpo
        for s in range(seqs):
            lines = slice(s * length, (s + 1) * length)
            part = jnp.dot(active[lines, :], buf_d[owner], preferred_element_type=F32)
            parts_d[owner, lines, :] = (part * buf_s[owner, 1:2, :]).astype(BF16)

            @pl.when(r != 0)
            def _():
                pltpu.make_async_remote_copy(
                    src_ref=parts_d.at[owner, lines], dst_ref=recv_d.at[r - 1, b, lines],
                    send_sem=down_send.at[owner, s], recv_sem=down_recv.at[r - 1, b, s],
                    device_id={"tp": t}, device_id_type=MESH,
                ).start()

    arrive(D, 2)
    down(fs)
    for k in range(1, hi + 1):
        if k > 2:
            arrive(D, k)
        down(member(pos - k))
        if (2 * k) % n:
            down(member(pos + k))

    ends = []
    for r in range(1, n_tp):
        for b in range(bpo):
            owner = (me + r) % n_tp * bpo + b
            for s in range(seqs):
                lines = slice(s * length, (s + 1) * length)
                ends.append(
                    to_peer(
                        parts_d.at[owner, lines], recv_d.at[r - 1, b, lines],
                        down_send.at[owner, s], down_recv.at[r - 1, b, s], r,
                    )
                )
    for copy in ends:
        copy.wait_recv()

    def store_out(at, cols, values):
        out[at, cols] = values

    total_of(
        lambda at, cols: rg[me, at, cols], lambda b, at: parts_d[me * bpo + b, at, :], recv_d,
        store_out,
    )

    for copy in tok_copies + mix_copies + res_copies + ends:
        copy.wait_send()
    for g in range(5):
        for h in (0, 1):
            for d in (0, 1):
                for k in range(1, hops(h, d) + 1):
                    ring(g, h, d, k).wait_send()


def on_device(
    n,
    n_tp,
    tokens,
    mix_gain,
    w_bgate,
    w_cgate,
    w_value,
    in_scale,
    mix_taps,
    w_mixout,
    mixout_scale,
    ffn_gain,
    w_upgate,
    w_upval,
    up_scale,
    ffn_taps,
    w_down,
    down_scale,
):
    seqs, length, own = tokens.shape
    rows = seqs * length
    width = own * n_tp
    part = w_bgate.shape[0]
    ff = w_upgate.shape[1]
    pad = -ff % 128
    ffp = ff + pad
    bw = w_mixout.shape[1]

    if pad:
        w_upgate, w_upval, up_scale, ffn_taps = (
            jnp.pad(x, [(0, 0)] * (x.ndim - 1) + [(0, pad)])
            for x in (w_upgate, w_upval, up_scale, ffn_taps)
        )
        w_down = jnp.pad(w_down, ((0, pad), (0, 0)))
    weights = (w_bgate, w_cgate, w_value, w_mixout, w_upgate, w_upval, w_down)
    held = [(16, bw), (part, 3 * own), w_mixout.shape, (part, 2 * ffp), w_down.shape]
    bpo = n // n_tp
    hi = n // 2
    vmem, dma = pltpu.VMEM, pltpu.SemaphoreType.DMA
    result = pl.pallas_call(
        functools.partial(layer_kernel, n, n_tp, seqs),
        out_shape=jax.ShapeDtypeStruct((rows, own), BF16),
        in_specs=[pl.BlockSpec(memory_space=pltpu.VMEM)] * 9
        + [pl.BlockSpec(memory_space=pl.ANY)] * 7,
        out_specs=pl.BlockSpec(memory_space=pltpu.VMEM),
        scratch_shapes=[vmem((n, *shape), BF16 if i else F32) for i, shape in enumerate(held)]
        + [vmem(w.shape, F32) for w in weights]
        + [
            vmem((n_tp, rows, own), BF16),
            vmem((n_tp, rows, own), BF16),
            vmem((rows, width), BF16),
            vmem((rows, own), BF16),
            vmem((rows, ffp), BF16),
            vmem((n, rows, bw), BF16),
            vmem((n_tp - 1, bpo, rows, bw), BF16),
            vmem((n, rows, bw), BF16),
            vmem((n_tp - 1, bpo, rows, bw), BF16),
            dma((5, 2, 2, hi)),
            dma((5, 2, 2, hi)),
            dma((n_tp - 1,)),
            dma((n_tp - 1,)),
            dma((n_tp - 1, bpo)),
            dma((n_tp - 1, bpo)),
            dma((n_tp - 1,)),
            dma((n_tp - 1,)),
            dma((n, seqs)),
            dma((n_tp - 1, bpo, seqs)),
            dma((7,)),
        ],
        compiler_params=pltpu.CompilerParams(
            collective_id=0, has_side_effects=True, vmem_limit_bytes=67043328
        ),
        name="layer",
    )(
        tokens.reshape(rows, own), mix_gain.reshape(1, width), ffn_gain.reshape(1, width),
        in_scale, mix_taps, up_scale, ffn_taps, mixout_scale, down_scale, *weights,
    )
    return result.reshape(seqs, length, own)


def solution(mesh):
    in_specs = (
        P("fs", None, "tp"),
        P(),
        P("fs", "tp"),
        P("fs", "tp"),
        P("fs", "tp"),
        P(None, "tp"),
        P(None, "tp"),
        P("tp", "fs"),
        P(None, "fs"),
        P(),
        P("fs", "tp"),
        P("fs", "tp"),
        P(None, "tp"),
        P(None, None, "tp"),
        P("tp", "fs"),
        P(None, "fs"),
    )
    out_specs = P("fs", None, "tp")
    body = functools.partial(on_device, mesh.shape["fs"], mesh.shape["tp"])
    return jax.shard_map(body, mesh=mesh, in_specs=in_specs, out_specs=out_specs, check_vma=False)
```
